32 devices in a mesh: sp: 8 (over z, y), dp: 4 (over x, core).
Axes of the slice: x: 2, y: 2, z: 4, core: 2. Of those that a mesh axis runs over, the one named last changes fastest.
Arguments:
- tokens: bfloat16 [4, 1024, 2048], P('dp', 'sp'), may hold values from -6 to 6
- cotangent: bfloat16 [4, 1024, 2048], P('dp', 'sp'), may hold values from -6 to 6
- value_weight: bfloat16 [2048, 2048], P(('sp', 'dp')), may hold values from -0.125 to 0.125
- query_heads: bfloat16 [4, 1024, 16, 128], P('dp', None, 'sp'), may hold values from -8 to 8
- key_heads: bfloat16 [4, 1024, 16, 128], P('dp', None, 'sp'), may hold values from -8 to 8
- lambdas: float32 [16], P('sp'), may hold values from 0.3 to 0.8
Outputs:
- grad_query: bfloat16 [4, 1024, 16, 128], P('dp', None, 'sp')
- grad_key: bfloat16 [4, 1024, 16, 128], P('dp', None, 'sp')
- grad_tokens: bfloat16 [4, 1024, 2048], P('dp', 'sp')
- grad_value_weight: float32 [2048, 2048], P(('sp', 'dp'))
- grad_lambda: float32 [16], P('sp')
The draws below stay inside these ranges and needn't reach their ends.
All inputs are finite; a program needn't handle non-finite values.
Results may differ from the reference program's by a relative error of at most 0.0095.
Values may be sent and summed in bfloat16 or wider, within the bound.
A program may use at most 192 MiB of HBM per device.

```python
import jax
import jax.numpy as jnp
from jax import lax

D = 2048
HEADS = 16
HEAD_DIM = 64
QBLOCK = 256
SEQS = 4
LENGTH = 1024
FEATURES = 2048


def pair_heads(key):
    array_shape = (SEQS, LENGTH, HEADS, 2 * HEAD_DIM)
    key_first = jax.random.fold_in(key, 11)
    key_second = jax.random.fold_in(key, 12)
    keys_part = jnp.clip(jax.random.normal(key_first, array_shape, jnp.float32) * 1.32, -8.0, 8.0)
    query_part = jnp.clip(jax.random.normal(key_second, array_shape, jnp.float32) * 1.32, -8.0, 8.0)
    return (query_part, keys_part)


def draw_query_heads(key, part):
    return pair_heads(key)[0].astype(jnp.bfloat16)


def draw_key_heads(key, part):
    return pair_heads(key)[1].astype(jnp.bfloat16)


def spiked(array, own_key, source, target, blocks, factor):
    def block_of(position):
        return (jnp.arange(array.shape[position]) // (array.shape[position] // blocks)).reshape((-1,) + (1,) * (array.ndim - 1 - position))

    first = jax.random.permutation(own_key, blocks)[block_of(target)]
    second = (block_of(target) + blocks // 2) % blocks
    return jnp.where((block_of(source) == first) | (block_of(source) == second), factor * array, array)


def block_levels(stream_key, shape, split, smallest, top_value):
    level, own = 1.0, jax.random.fold_in(stream_key, 6)
    for dim, blocks in split:
        steps = jnp.exp(jax.random.uniform(jax.random.fold_in(own, dim), (blocks,), jnp.float32, smallest / len(split), top_value / len(split)))
        level = level * jnp.repeat(steps, shape[dim] // blocks).reshape([-1 if axis == dim else 1 for axis in range(len(shape))])
    return level


def noise(own_key, shape, spread, limit, split=(), held_as=jnp.bfloat16):
    loudness = block_levels(own_key, shape, split, -0.22, 0.18) if split else 1.0
    values = jax.random.normal(own_key, shape, jnp.float32) * spread * loudness
    return jnp.minimum(jnp.maximum(values, -limit), limit).astype(held_as)


def bell_draw_with(rng, dims, deviation, reach, cuts, heavy, kind=jnp.bfloat16):
    drawn = deviation * jax.random.normal(rng, dims, jnp.float32)
    if cuts:
        drawn = drawn * block_levels(rng, dims, cuts, -0.22, 0.18)
    return jnp.clip(spiked(drawn, jax.random.fold_in(rng, 3), *heavy), -reach, reach).astype(kind)


def setup_inputs(seed: int = 0) -> dict:
    key_of = jax.random.split(jax.random.key(seed), 7)
    tokens = bell_draw_with(key_of[0], (SEQS, LENGTH, D), 1.0, 6.0, ((0, 4), (1, 8)), (1, 2, 8, 2.0))
    cotangent = noise(key_of[1], (SEQS, LENGTH, FEATURES), 1.0, 6.0, ((0, 4), (1, 8)))
    value_weight = noise(key_of[2], (D, FEATURES), D ** -0.5, 0.125, ((0, 32),))
    query_heads = draw_query_heads(jax.random.fold_in(key_of[6], 71), 0)
    key_heads = draw_key_heads(jax.random.fold_in(key_of[6], 71), 0)
    lambdas = jnp.clip(0.3 + 0.5 * jax.random.uniform(key_of[5], (HEADS,), jnp.float32) ** block_levels(key_of[5], (HEADS,), ((0, 8),), -0.2, 0.2), 0.3, 0.8)
    return {"tokens": tokens, "cotangent": cotangent, "value_weight": value_weight, "query_heads": query_heads, "key_heads": key_heads, "lambdas": lambdas}


EPS = 1e-06
NEGATIVE = -1e+30

def head_backward(queries, keys_in, values_in, cotangent, lambdas, block_rows):
    seq_length = queries.shape[0]
    head_count = queries.shape[1]
    head_width = queries.shape[3]
    scaling = head_width ** (-0.5)
    blocks_count = seq_length // block_rows
    positions = jnp.arange(seq_length, dtype=jnp.int32)
    keys_wide = keys_in.astype(jnp.float32)
    values_wide = values_in.astype(jnp.float32)
    lambda_col = lambdas[:, None, None]

    def block_step(totals, block_index):
        grad_key_sum, grad_value_sum, grad_lambda_sum = totals
        offset = (block_index * block_rows).astype(jnp.int32)
        query_block = lax.dynamic_slice_in_dim(queries, offset, block_rows, 0).astype(jnp.float32)
        cotan_block = lax.dynamic_slice_in_dim(cotangent, offset, block_rows, 0).astype(jnp.float32)
        scores = jnp.einsum('qhcd,khcd->hcqk', query_block, keys_wide) * scaling
        rows_pos = offset + jnp.arange(block_rows, dtype=jnp.int32)
        allowed = rows_pos[:, None] >= positions[None, :]
        scores = jnp.where(allowed, scores, NEGATIVE)
        highest = lax.optimization_barrier(jnp.max(scores, axis=-1, keepdims=True))
        exponent = jnp.exp(scores - highest)
        softmaxes = exponent / lax.optimization_barrier(jnp.sum(exponent, axis=-1, keepdims=True))
        weights = (softmaxes[:, 0] - lambda_col * softmaxes[:, 1]).astype(jnp.bfloat16)
        weights_wide = weights.astype(jnp.float32)
        mixed_out = jnp.einsum('hqk,khd->qhd', weights_wide, values_wide)
        inverse = lax.rsqrt(lax.optimization_barrier(jnp.mean(mixed_out * mixed_out, axis=-1, keepdims=True)) + EPS)
        normed = mixed_out * inverse
        grad_mixed = (inverse * (cotan_block - normed * lax.optimization_barrier(jnp.mean(cotan_block * normed, axis=-1, keepdims=True)))).astype(jnp.bfloat16)
        grad_mixed_wide = grad_mixed.astype(jnp.float32)
        grad_weights = jnp.einsum('qhd,khd->hqk', grad_mixed_wide, values_wide)
        grad_value_sum = grad_value_sum + jnp.einsum('hqk,qhd->khd', weights_wide, grad_mixed_wide)
        grad_lambda_sum = grad_lambda_sum - lax.optimization_barrier(jnp.sum(grad_weights * softmaxes[:, 1], axis=(1, 2)))
        first_grad = softmaxes[:, 0] * (grad_weights - lax.optimization_barrier(jnp.sum(grad_weights * softmaxes[:, 0], axis=-1, keepdims=True)))
        second_grad = -lambda_col * softmaxes[:, 1] * (grad_weights - lax.optimization_barrier(jnp.sum(grad_weights * softmaxes[:, 1], axis=-1, keepdims=True)))
        grad_scores = (jnp.stack([first_grad, second_grad], axis=1) * scaling).astype(jnp.bfloat16)
        grad_scores_wide = grad_scores.astype(jnp.float32)
        grad_query_block = jnp.einsum('hcqk,khcd->qhcd', grad_scores_wide, keys_wide).astype(jnp.bfloat16)
        grad_key_sum = grad_key_sum + jnp.einsum('hcqk,qhcd->khcd', grad_scores_wide, query_block)
        return ((grad_key_sum, grad_value_sum, grad_lambda_sum), grad_query_block)
    initial = (jnp.zeros(keys_in.shape, jnp.float32), jnp.zeros(values_in.shape, jnp.float32), jnp.zeros((head_count,), jnp.float32))
    totals, query_blocks = lax.scan(block_step, initial, jnp.arange(blocks_count, dtype=jnp.int32))
    grad_query = query_blocks.reshape(queries.shape)
    return (grad_query, totals[0].astype(jnp.bfloat16), totals[1].astype(jnp.bfloat16), totals[2])

def reference(tokens, cotangent, value_weight, query_heads, key_heads, lambdas):
    seq_count = tokens.shape[0]
    seq_length = tokens.shape[1]
    feature_count = value_weight.shape[1]
    flat_tokens = tokens.reshape(seq_count * seq_length, D)
    values_flat = jnp.dot(flat_tokens, value_weight, preferred_element_type=jnp.float32).astype(jnp.bfloat16)
    values_heads = values_flat.reshape(seq_count, seq_length, HEADS, 2 * HEAD_DIM)
    cotan_heads = cotangent.reshape(seq_count, seq_length, HEADS, 2 * HEAD_DIM)
    queries = query_heads.reshape(seq_count, seq_length, HEADS, 2, HEAD_DIM)
    keys_in = key_heads.reshape(seq_count, seq_length, HEADS, 2, HEAD_DIM)

    def one_sequence(items):
        return head_backward(items[0], items[1], items[2], items[3], lambdas, QBLOCK)
    grad_query, grad_key, grad_value, grad_lambda = lax.map(one_sequence, (queries, keys_in, values_heads, cotan_heads))
    grad_lambda = lax.optimization_barrier(jnp.sum(grad_lambda, axis=0))
    grad_flat = grad_value.reshape(seq_count * seq_length, feature_count)
    grad_tokens = jnp.dot(grad_flat, value_weight.T, preferred_element_type=jnp.float32).astype(jnp.bfloat16)
    grad_weight = jnp.dot(flat_tokens.T, grad_flat, preferred_element_type=jnp.float32)
    return (grad_query.reshape(query_heads.shape), grad_key.reshape(key_heads.shape), grad_tokens.reshape(tokens.shape), grad_weight, grad_lambda)
```

```python
import functools

import jax
import jax.numpy as jnp
from jax import lax
from jax.experimental import pallas as pl
from jax.experimental.pallas import tpu as pltpu
from jax.sharding import PartitionSpec as P

QBLOCK = 256
EPS = 1e-06
NEGATIVE = -1e30
CHUNKS = 2
F32 = jnp.float32
BF16 = jnp.bfloat16


def dot_nn(a, b):
    return jnp.dot(a, b, preferred_element_type=F32)


def dot_nt(a, b):
    return lax.dot_general(a, b, (((1,), (1,)), ((), ())), preferred_element_type=F32)


def attention_kernel(
    lam_ref, q_ref, k_ref, v_ref, g_ref, gq_ref, gk_ref, gv_ref, gl_ref, gk_acc, gv_acc
):
    length, width = q_ref.shape
    half = width // 2
    block = min(QBLOCK, length)
    scaling = half ** (-0.5)
    lam = lam_ref[pl.program_id(0)]
    lanes = lax.broadcasted_iota(jnp.int32, (length, width), 1)
    first_half = lanes < half
    q_all = q_ref[...].astype(F32) * scaling
    k_all = k_ref[...].astype(F32) * scaling
    q_halves = [
        jnp.where(first_half, q_all, 0.0).astype(BF16),
        jnp.where(first_half, 0.0, q_all).astype(BF16),
    ]
    kt_halves = [
        jnp.where(first_half, k_all, 0.0).T.astype(BF16),
        jnp.where(first_half, 0.0, k_all).T.astype(BF16),
    ]
    vt = v_ref[...].astype(F32).T.astype(BF16)
    gt = g_ref[...].astype(F32).T
    keep = lax.broadcasted_iota(jnp.int32, (block, block), 0) <= lax.broadcasted_iota(
        jnp.int32, (block, block), 1
    )
    lambda_total = jnp.zeros((1, block), F32)
    for index in range(length // block):
        off = index * block
        reach = off + block
        pieces = ([(0, off)] if off else []) + [(off, reach)]
        probs = []
        for c in range(2):
            qc = q_halves[c][off:reach]
            scores = [dot_nt(k_ref[lo:hi], qc) for lo, hi in pieces]
            scores[-1] = jnp.where(keep, scores[-1], NEGATIVE)
            top = functools.reduce(
                jnp.maximum, [jnp.max(s, axis=0, keepdims=True) for s in scores]
            )
            exps = [jnp.exp(s - top) for s in scores]
            total = sum(jnp.sum(e, axis=0, keepdims=True) for e in exps)
            inv = 1.0 / total
            probs.append([e * inv for e in exps])
        weights = [(p1 - lam * p2).astype(BF16) for p1, p2 in zip(*probs)]
        out_t = sum(dot_nn(vt[:, lo:hi], w) for (lo, hi), w in zip(pieces, weights))
        cot = gt[:, off:reach]
        inverse = lax.rsqrt(jnp.mean(out_t * out_t, axis=0, keepdims=True) + EPS)
        normed = out_t * inverse
        grad_out = (
            inverse * (cot - normed * jnp.mean(cot * normed, axis=0, keepdims=True))
        ).astype(BF16)
        grad_w = [dot_nn(v_ref[lo:hi], grad_out) for lo, hi in pieces]
        sums = [
            sum(jnp.sum(d * p, axis=0, keepdims=True) for d, p in zip(grad_w, probs[c]))
            for c in range(2)
        ]
        lambda_total = lambda_total - sums[1]
        first = [(p * (d - sums[0])).astype(BF16) for d, p in zip(grad_w, probs[0])]
        second = [(-lam * p * (d - sums[1])).astype(BF16) for d, p in zip(grad_w, probs[1])]
        gq_t = sum(
            dot_nn(kt_halves[0][:, lo:hi], a) + dot_nn(kt_halves[1][:, lo:hi], b)
            for (lo, hi), a, b in zip(pieces, first, second)
        )
        gq_ref[off:reach, :] = gq_t.T.astype(BF16)
        for (lo, hi), w, a, b in zip(pieces, weights, first, second):
            gv = dot_nt(w, grad_out)
            gk = dot_nn(a, q_halves[0][off:reach]) + dot_nn(b, q_halves[1][off:reach])
            if lo == off:
                gv_acc[lo:hi, :] = gv
                gk_acc[lo:hi, :] = gk
            else:
                gv_acc[lo:hi, :] += gv
                gk_acc[lo:hi, :] += gk
    gk_ref[...] = gk_acc[...].astype(BF16)
    gv_ref[...] = gv_acc[...].astype(BF16)
    gl_ref[...] = jnp.broadcast_to(jnp.sum(lambda_total, axis=1, keepdims=True), gl_ref.shape[1:])[
        None
    ]


def attention(lambdas, queries, keys, values, cotangent, width):
    length, features = queries.shape
    heads = features // width
    column = pl.BlockSpec((length, width), lambda h: (0, h))
    shape = jax.ShapeDtypeStruct((length, features), BF16)
    return pl.pallas_call(
        attention_kernel,
        grid=(heads,),
        in_specs=[pl.BlockSpec(memory_space=pltpu.SMEM)] + [column] * 4,
        out_specs=[column] * 3 + [pl.BlockSpec((1, 8, 128), lambda h: (h, 0, 0))],
        out_shape=[shape] * 3 + [jax.ShapeDtypeStruct((heads, 8, 128), F32)],
        scratch_shapes=[pltpu.VMEM((length, width), F32)] * 2,
        compiler_params=pltpu.CompilerParams(vmem_limit_bytes=48 * 1024 * 1024),
        cost_estimate=pl.CostEstimate(
            flops=12 * length * length * width * heads,
            bytes_accessed=14 * length * features,
            transcendentals=length * length * heads,
        ),
        name="attention",
    )(lambdas, queries, keys, values, cotangent)


def remote(src, dst, send, recv, sp, dp):
    return pltpu.make_async_remote_copy(
        src_ref=src,
        dst_ref=dst,
        send_sem=send,
        recv_sem=recv,
        device_id=(sp, dp),
        device_id_type=pl.DeviceIdType.MESH,
    )


def ring_place(sp, n):
    odd = sp % 2
    return (1 - odd) * (sp // 2) + odd * (n - 1 - sp // 2)


def ring_member(place, n):
    late = place // (n // 2)
    return (1 - late) * (2 * place) + late * (2 * (n - 1 - place) + 1)


def greet(peers):
    barrier = pltpu.get_barrier_semaphore()
    for sp, dp in peers:
        pl.semaphore_signal(
            barrier, inc=1, device_id=(sp, dp), device_id_type=pl.DeviceIdType.MESH
        )
    pl.semaphore_wait(barrier, len(peers))


def gather_kernel(
    n,
    m,
    tok_ref,
    cot_ref,
    w_ref,
    all_ref,
    coth_ref,
    wc_ref,
    local_sem,
    ring_send,
    ring_recv,
    a_send,
    a_recv,
    x_send,
    x_recv,
    c_send,
    c_recv,
):
    me = lax.axis_index("sp")
    my_dp = lax.axis_index("dp")
    rows = tok_ref.shape[0]
    feats = coth_ref.shape[2]
    part = rows // (2 * CHUNKS)
    place = ring_place(me, n)
    sides = [
        ring_member((place + 1) % n, n),
        ring_member((place + n - 1) % n, n),
    ]
    core = my_dp + 1 - 2 * (my_dp % 2)
    sp_peers = [(me + k) % n for k in range(1, n)]
    x_peers = [(my_dp + 2 * k) % m for k in range(1, m // 2)]
    greet(
        [(s, my_dp) for s in sp_peers] + [(me, d) for d in x_peers] + [(me, core)]
    )

    def columns(ref, s):
        return ref.at[:, pl.ds(pl.multiple_of(s * feats, feats), feats)]

    w_copies = [
        remote(columns(w_ref, s), wc_ref.at[me, my_dp], a_send.at[0, k], a_recv.at[0, k], s, my_dp)
        for k, s in enumerate(sp_peers)
    ]
    for copy in w_copies:
        copy.start()

    def ring(step, side, chunk):
        origin = (place + n - step) % n if side == 0 else (place + step) % n
        block = ring_member(origin, n)
        span = pl.ds((side * CHUNKS + chunk) * part, part)
        src = tok_ref.at[span] if step == 0 else all_ref.at[block, span]
        return remote(
            src,
            all_ref.at[block, span],
            ring_send.at[step, side, chunk],
            ring_recv.at[step, side, chunk],
            sides[side],
            my_dp,
        )

    order = [(side, chunk) for chunk in range(CHUNKS) for side in range(2)]
    hops = {}
    for side, chunk in order:
        hops[0, side, chunk] = ring(0, side, chunk)
        hops[0, side, chunk].start()
    locals_ = [
        pltpu.make_async_copy(tok_ref, all_ref.at[me], local_sem.at[0]),
        pltpu.make_async_copy(columns(cot_ref, me), coth_ref.at[me], local_sem.at[1]),
        pltpu.make_async_copy(columns(w_ref, me), wc_ref.at[me, my_dp], local_sem.at[2]),
    ]
    for copy in locals_:
        copy.start()
    cot_copies = [
        remote(columns(cot_ref, s), coth_ref.at[me], a_send.at[1, k], a_recv.at[1, k], s, my_dp)
        for k, s in enumerate(sp_peers)
    ]
    for copy in cot_copies:
        copy.start()
    locals_[2].wait()
    for copy in w_copies:
        copy.wait_recv()
    x_copies = [
        remote(wc_ref.at[:, my_dp], wc_ref.at[:, my_dp], x_send.at[k], x_recv.at[k], me, d)
        for k, d in enumerate(x_peers)
    ]
    for copy in x_copies:
        copy.start()
    c_copies = [remote(wc_ref.at[:, my_dp], wc_ref.at[:, my_dp], c_send.at[0], c_recv.at[0], me, core)]
    c_copies[0].start()
    for step in range(1, n - 1):
        for side, chunk in order:
            hops[step - 1, side, chunk].wait_recv()
            hops[step, side, chunk] = ring(step, side, chunk)
            hops[step, side, chunk].start()
        if step == n // 2:
            for k in range(1, m // 2):
                origin = (my_dp + m - 2 * k) % m
                x_copies[k - 1].wait_recv()
                copy = remote(
                    wc_ref.at[:, origin], wc_ref.at[:, origin], c_send.at[k], c_recv.at[k], me, core
                )
                copy.start()
                c_copies.append(copy)
    for side, chunk in order:
        hops[n - 2, side, chunk].wait_recv()
    for copy in cot_copies + c_copies:
        copy.wait_recv()
    for copy in list(hops.values()) + w_copies + cot_copies + x_copies + c_copies:
        copy.wait_send()
    locals_[0].wait()
    locals_[1].wait()


def gather(tokens, cotangent, weight, n, m):
    rows, depth = tokens.shape
    feats = weight.shape[1] // n
    vmem = pl.BlockSpec(memory_space=pltpu.VMEM)
    dma = pltpu.SemaphoreType.DMA
    return pl.pallas_call(
        functools.partial(gather_kernel, n, m),
        out_shape=[
            jax.ShapeDtypeStruct((n, rows, depth), BF16),
            jax.ShapeDtypeStruct((n, rows, feats), BF16),
            jax.ShapeDtypeStruct((n, m, weight.shape[0], feats), BF16),
        ],
        in_specs=[vmem] * 3,
        out_specs=[vmem] * 3,
        scratch_shapes=[
            dma((3,)),
            dma((n - 1, 2, CHUNKS)),
            dma((n - 1, 2, CHUNKS)),
            dma((2, n - 1)),
            dma((2, n - 1)),
            dma((max(m // 2 - 1, 1),)),
            dma((max(m // 2 - 1, 1),)),
            dma((m // 2,)),
            dma((m // 2,)),
        ],
        compiler_params=pltpu.CompilerParams(
            collective_id=0, has_side_effects=True, vmem_limit_bytes=40 * 1024 * 1024
        ),
        cost_estimate=pl.CostEstimate(
            flops=40_000_000_000, bytes_accessed=20_000_000, transcendentals=0
        ),
        name="gather",
    )(tokens, cotangent, weight)


def scatter_kernel(
    n, m, dv_ref, t_ref, gl_ref, dvt_ref, gw_ref, glo_ref, rbuf, sbuf, fbuf, lbuf,
    local_sem, v_send, v_recv, t_send, t_recv, l_send, l_recv, f_send, f_recv,
):
    me = lax.axis_index("sp")
    my_dp = lax.axis_index("dp")
    rows = dvt_ref.shape[0]
    feats = dv_ref.shape[1]
    sp_peers = [(me + k) % n for k in range(1, n)]
    dp_peers = [(my_dp + k) % m for k in range(1, m)]
    greet([(s, my_dp) for s in sp_peers] + [(me, d) for d in dp_peers])

    def tokens_of(s):
        return dv_ref.at[pl.ds(pl.multiple_of(s * rows, rows), rows)]

    mine = dvt_ref.at[:, pl.ds(pl.multiple_of(me * feats, feats), feats)]
    t_copies = [
        remote(t_ref.at[d], rbuf.at[k], t_send.at[k], t_recv.at[k], me, d)
        for k, d in enumerate(dp_peers)
    ]
    l_copies = [
        remote(gl_ref, lbuf.at[k], l_send.at[k], l_recv.at[k], me, d)
        for k, d in enumerate(dp_peers)
    ]
    v_copies = [
        remote(tokens_of(s), mine, v_send.at[k], v_recv.at[k], s, my_dp)
        for k, s in enumerate(sp_peers)
    ]
    for copy in l_copies + t_copies + v_copies:
        copy.start()
    own = pltpu.make_async_copy(tokens_of(me), mine, local_sem.at[0])
    own.start()
    for copy in t_copies:
        copy.wait_recv()
    total = t_ref[my_dp].astype(F32)
    for k in range(m - 1):
        total = total + rbuf[k].astype(F32)
    sbuf[...] = total.astype(BF16)
    f_copies = [
        remote(sbuf.at[s], fbuf.at[me], f_send.at[k], f_recv.at[k], s, my_dp)
        for k, s in enumerate(sp_peers)
    ]
    for copy in f_copies:
        copy.start()
    own_f = pltpu.make_async_copy(sbuf.at[me], fbuf.at[me], local_sem.at[1])
    own_f.start()
    for copy in l_copies:
        copy.wait_recv()
    lam = gl_ref[...]
    for k in range(m - 1):
        lam = lam + lbuf[k]
    glo_ref[...] = lam
    own_f.wait()
    for copy in f_copies:
        copy.wait_recv()
    for s in range(n):
        gw_ref[:, s * feats : (s + 1) * feats] = fbuf[s].astype(F32)
    own.wait()
    for copy in v_copies:
        copy.wait_recv()
    for copy in l_copies + t_copies + v_copies + f_copies:
        copy.wait_send()


def scatter(grad_value, term, grad_lambda, n, m):
    length, feats = grad_value.shape
    row_count = term.shape[2]
    vmem = pl.BlockSpec(memory_space=pltpu.VMEM)
    dma = pltpu.SemaphoreType.DMA
    return pl.pallas_call(
        functools.partial(scatter_kernel, n, m),
        out_shape=[
            jax.ShapeDtypeStruct((length // n, n * feats), BF16),
            jax.ShapeDtypeStruct((row_count, n * feats), F32),
            jax.ShapeDtypeStruct(grad_lambda.shape, F32),
        ],
        in_specs=[vmem] * 3,
        out_specs=[vmem] * 3,
        scratch_shapes=[
            pltpu.VMEM((m - 1,) + term.shape[1:], BF16),
            pltpu.VMEM(term.shape[1:], BF16),
            pltpu.VMEM(term.shape[1:], BF16),
            pltpu.VMEM((m - 1,) + grad_lambda.shape, F32),
            dma((2,)),
            dma((n - 1,)),
            dma((n - 1,)),
            dma((m - 1,)),
            dma((m - 1,)),
            dma((m - 1,)),
            dma((m - 1,)),
            dma((n - 1,)),
            dma((n - 1,)),
        ],
        compiler_params=pltpu.CompilerParams(
            collective_id=1, has_side_effects=True, vmem_limit_bytes=40 * 1024 * 1024
        ),
        name="scatter",
    )(grad_value, term, grad_lambda)


def body(n, m, tokens, cotangent, value_weight, query_heads, key_heads, lambdas):
    row_count, feature_count = value_weight.shape
    all_weight = lax.all_gather(value_weight, ("sp", "dp"), axis=0, tiled=True)
    all_tokens, cotan_heads, weight_cols = gather(tokens[0], cotangent[0], value_weight, n, m)
    feats = feature_count // n
    depth = n * m * row_count
    length = all_tokens.shape[0] * all_tokens.shape[1]
    head_count, width = query_heads.shape[2], query_heads.shape[3]
    flat_tokens = all_tokens.reshape(length, depth)
    values = jnp.dot(
        flat_tokens, weight_cols.reshape(depth, feats), preferred_element_type=F32
    ).astype(BF16)
    grad_query, grad_key, grad_value, grad_lambda = attention(
        lambdas,
        query_heads.reshape(length, feats),
        key_heads.reshape(length, feats),
        values,
        cotan_heads.reshape(length, feats),
        width,
    )
    term = lax.dot_general(
        flat_tokens, grad_value, (((0,), (0,)), ((), ())), preferred_element_type=F32
    ).astype(BF16)
    term = term.reshape(n, m, row_count, feats).transpose(1, 0, 2, 3)
    grad_value_tokens, grad_weight, lambda_sum = scatter(grad_value, term, grad_lambda, n, m)
    grad_tokens = dot_nt(grad_value_tokens, all_weight).astype(BF16)[None]
    return (
        grad_query.reshape(1, length, head_count, width),
        grad_key.reshape(1, length, head_count, width),
        grad_tokens,
        grad_weight,
        lambda_sum[:, 0, 0],
    )


def solution(mesh):
    placed = (
        P("dp", "sp", None),
        P("dp", "sp", None),
        P(("sp", "dp"), None),
        P("dp", None, "sp", None),
        P("dp", None, "sp", None),
        P("sp"),
    )
    return jax.shard_map(
        functools.partial(body, mesh.shape["sp"], mesh.shape["dp"]),
        mesh=mesh,
        in_specs=placed,
        out_specs=(
            P("dp", None, "sp", None),
            P("dp", None, "sp", None),
            P("dp", "sp", None),
            P(("sp", "dp"), None),
            P("sp"),
        ),
        check_vma=False,
    )
```

```python
import functools

import jax
import jax.numpy as jnp
from jax import lax
from jax.experimental import pallas as pl
from jax.experimental.pallas import tpu as pltpu
from jax.sharding import PartitionSpec as P

QBLOCK = 256
EPS = 1e-06
NEGATIVE = -1e30
CHUNKS = 2
F32 = jnp.float32
BF16 = jnp.bfloat16


def dot_nn(a, b):
    return jnp.dot(a, b, preferred_element_type=F32)


def dot_nt(a, b):
    return lax.dot_general(a, b, (((1,), (1,)), ((), ())), preferred_element_type=F32)


def attention_kernel(
    lam_ref, q_ref, k_ref, v_ref, g_ref, gq_ref, gk_ref, gv_ref, gl_ref, gk_acc, gv_acc
):
    length, width = q_ref.shape
    half = width // 2
    block = min(QBLOCK, length)
    scaling = half ** (-0.5)
    lam = lam_ref[pl.program_id(0)]
    lanes = lax.broadcasted_iota(jnp.int32, (length, width), 1)
    first_half = lanes < half
    q_all = q_ref[...].astype(F32) * scaling
    k_all = k_ref[...].astype(F32) * scaling
    q_halves = [
        jnp.where(first_half, q_all, 0.0).astype(BF16),
        jnp.where(first_half, 0.0, q_all).astype(BF16),
    ]
    kt_halves = [
        jnp.where(first_half, k_all, 0.0).T.astype(BF16),
        jnp.where(first_half, 0.0, k_all).T.astype(BF16),
    ]
    vt = v_ref[...].astype(F32).T.astype(BF16)
    gt = g_ref[...].astype(F32).T
    keep = lax.broadcasted_iota(jnp.int32, (block, block), 0) <= lax.broadcasted_iota(
        jnp.int32, (block, block), 1
    )
    lambda_total = jnp.zeros((1, block), F32)
    for index in range(length // block):
        off = index * block
        reach = off + block
        pieces = ([(0, off)] if off else []) + [(off, reach)]
        probs = []
        for c in range(2):
            qc = q_halves[c][off:reach]
            scores = [dot_nt(k_ref[lo:hi], qc) for lo, hi in pieces]
            scores[-1] = jnp.where(keep, scores[-1], NEGATIVE)
            top = functools.reduce(
                jnp.maximum, [jnp.max(s, axis=0, keepdims=True) for s in scores]
            )
            exps = [jnp.exp(s - top) for s in scores]
            total = sum(jnp.sum(e, axis=0, keepdims=True) for e in exps)
            inv = 1.0 / total
            probs.append([e * inv for e in exps])
        weights = [(p1 - lam * p2).astype(BF16) for p1, p2 in zip(*probs)]
        out_t = sum(dot_nn(vt[:, lo:hi], w) for (lo, hi), w in zip(pieces, weights))
        cot = gt[:, off:reach]
        inverse = lax.rsqrt(jnp.mean(out_t * out_t, axis=0, keepdims=True) + EPS)
        normed = out_t * inverse
        grad_out = (
            inverse * (cot - normed * jnp.mean(cot * normed, axis=0, keepdims=True))
        ).astype(BF16)
        grad_w = [dot_nn(v_ref[lo:hi], grad_out) for lo, hi in pieces]
        sums = [
            sum(jnp.sum(d * p, axis=0, keepdims=True) for d, p in zip(grad_w, probs[c]))
            for c in range(2)
        ]
        lambda_total = lambda_total - sums[1]
        first = [(p * (d - sums[0])).astype(BF16) for d, p in zip(grad_w, probs[0])]
        second = [(-lam * p * (d - sums[1])).astype(BF16) for d, p in zip(grad_w, probs[1])]
        gq_t = sum(
            dot_nn(kt_halves[0][:, lo:hi], a) + dot_nn(kt_halves[1][:, lo:hi], b)
            for (lo, hi), a, b in zip(pieces, first, second)
        )
        gq_ref[off:reach, :] = gq_t.T.astype(BF16)
        for (lo, hi), w, a, b in zip(pieces, weights, first, second):
            gv = dot_nt(w, grad_out)
            gk = dot_nn(a, q_halves[0][off:reach]) + dot_nn(b, q_halves[1][off:reach])
            if lo == off:
                gv_acc[lo:hi, :] = gv
                gk_acc[lo:hi, :] = gk
            else:
                gv_acc[lo:hi, :] += gv
                gk_acc[lo:hi, :] += gk
    gk_ref[...] = gk_acc[...].astype(BF16)
    gv_ref[...] = gv_acc[...].astype(BF16)
    gl_ref[...] = jnp.broadcast_to(jnp.sum(lambda_total, axis=1, keepdims=True), gl_ref.shape[1:])[
        None
    ]


def attention(lambdas, queries, keys, values, cotangent, width):
    length, features = queries.shape
    heads = features // width
    column = pl.BlockSpec((length, width), lambda h: (0, h))
    shape = jax.ShapeDtypeStruct((length, features), BF16)
    return pl.pallas_call(
        attention_kernel,
        grid=(heads,),
        in_specs=[pl.BlockSpec(memory_space=pltpu.SMEM)] + [column] * 4,
        out_specs=[column] * 3 + [pl.BlockSpec((1, 8, 128), lambda h: (h, 0, 0))],
        out_shape=[shape] * 3 + [jax.ShapeDtypeStruct((heads, 8, 128), F32)],
        scratch_shapes=[pltpu.VMEM((length, width), F32)] * 2,
        compiler_params=pltpu.CompilerParams(vmem_limit_bytes=48 * 1024 * 1024),
        cost_estimate=pl.CostEstimate(
            flops=12 * length * length * width * heads,
            bytes_accessed=14 * length * features,
            transcendentals=length * length * heads,
        ),
        name="attention",
    )(lambdas, queries, keys, values, cotangent)


def remote(src, dst, send, recv, sp, dp):
    return pltpu.make_async_remote_copy(
        src_ref=src,
        dst_ref=dst,
        send_sem=send,
        recv_sem=recv,
        device_id=(sp, dp),
        device_id_type=pl.DeviceIdType.MESH,
    )


def ring_place(sp, n):
    odd = sp % 2
    return (1 - odd) * (sp // 2) + odd * (n - 1 - sp // 2)


def ring_member(place, n):
    late = place // (n // 2)
    return (1 - late) * (2 * place) + late * (2 * (n - 1 - place) + 1)


def greet(peers):
    barrier = pltpu.get_barrier_semaphore()
    for sp, dp in peers:
        pl.semaphore_signal(
            barrier, inc=1, device_id=(sp, dp), device_id_type=pl.DeviceIdType.MESH
        )
    pl.semaphore_wait(barrier, len(peers))


def gather_kernel(
    n,
    m,
    tok_ref,
    cot_ref,
    w_ref,
    all_ref,
    coth_ref,
    wc_ref,
    local_sem,
    ring_send,
    ring_recv,
    a_send,
    a_recv,
    x_send,
    x_recv,
    c_send,
    c_recv,
):
    me = lax.axis_index("sp")
    my_dp = lax.axis_index("dp")
    rows = tok_ref.shape[0]
    feats = coth_ref.shape[2]
    part = rows // (2 * CHUNKS)
    place = ring_place(me, n)
    sides = [
        ring_member((place + 1) % n, n),
        ring_member((place + n - 1) % n, n),
    ]
    core = my_dp + 1 - 2 * (my_dp % 2)
    sp_peers = [(me + k) % n for k in range(1, n)]
    x_peers = [(my_dp + 2 * k) % m for k in range(1, m // 2)]
    greet(
        [(s, my_dp) for s in sp_peers] + [(me, d) for d in x_peers] + [(me, core)]
    )

    def columns(ref, s):
        return ref.at[:, pl.ds(pl.multiple_of(s * feats, feats), feats)]

    w_copies = [
        remote(columns(w_ref, s), wc_ref.at[me, my_dp], a_send.at[0, k], a_recv.at[0, k], s, my_dp)
        for k, s in enumerate(sp_peers)
    ]
    for copy in w_copies:
        copy.start()

    def ring(step, side, chunk):
        origin = (place + n - step) % n if side == 0 else (place + step) % n
        block = ring_member(origin, n)
        span = pl.ds((side * CHUNKS + chunk) * part, part)
        src = tok_ref.at[span] if step == 0 else all_ref.at[block, span]
        return remote(
            src,
            all_ref.at[block, span],
            ring_send.at[step, side, chunk],
            ring_recv.at[step, side, chunk],
            sides[side],
            my_dp,
        )

    order = [(side, chunk) for chunk in range(CHUNKS) for side in range(2)]
    hops = {}
    for side, chunk in order:
        hops[0, side, chunk] = ring(0, side, chunk)
        hops[0, side, chunk].start()
    locals_ = [
        pltpu.make_async_copy(tok_ref, all_ref.at[me], local_sem.at[0]),
        pltpu.make_async_copy(columns(cot_ref, me), coth_ref.at[me], local_sem.at[1]),
        pltpu.make_async_copy(columns(w_ref, me), wc_ref.at[me, my_dp], local_sem.at[2]),
    ]
    for copy in locals_:
        copy.start()
    cot_copies = [
        remote(columns(cot_ref, s), coth_ref.at[me], a_send.at[1, k], a_recv.at[1, k], s, my_dp)
        for k, s in enumerate(sp_peers)
    ]
    for copy in cot_copies:
        copy.start()
    locals_[2].wait()
    for copy in w_copies:
        copy.wait_recv()
    x_copies = [
        remote(wc_ref.at[:, my_dp], wc_ref.at[:, my_dp], x_send.at[k], x_recv.at[k], me, d)
        for k, d in enumerate(x_peers)
    ]
    for copy in x_copies:
        copy.start()
    c_copies = [remote(wc_ref.at[:, my_dp], wc_ref.at[:, my_dp], c_send.at[0], c_recv.at[0], me, core)]
    c_copies[0].start()
    for step in range(1, n - 1):
        for side, chunk in order:
            hops[step - 1, side, chunk].wait_recv()
            hops[step, side, chunk] = ring(step, side, chunk)
            hops[step, side, chunk].start()
        if step == n // 2:
            for k in range(1, m // 2):
                origin = (my_dp + m - 2 * k) % m
                x_copies[k - 1].wait_recv()
                copy = remote(
                    wc_ref.at[:, origin], wc_ref.at[:, origin], c_send.at[k], c_recv.at[k], me, core
                )
                copy.start()
                c_copies.append(copy)
    for side, chunk in order:
        hops[n - 2, side, chunk].wait_recv()
    for copy in cot_copies + c_copies:
        copy.wait_recv()
    for copy in list(hops.values()) + w_copies + cot_copies + x_copies + c_copies:
        copy.wait_send()
    locals_[0].wait()
    locals_[1].wait()


def gather(tokens, cotangent, weight, n, m):
    rows, depth = tokens.shape
    feats = weight.shape[1] // n
    vmem = pl.BlockSpec(memory_space=pltpu.VMEM)
    dma = pltpu.SemaphoreType.DMA
    return pl.pallas_call(
        functools.partial(gather_kernel, n, m),
        out_shape=[
            jax.ShapeDtypeStruct((n, rows, depth), BF16),
            jax.ShapeDtypeStruct((n, rows, feats), BF16),
            jax.ShapeDtypeStruct((n, m, weight.shape[0], feats), BF16),
        ],
        in_specs=[vmem] * 3,
        out_specs=[vmem] * 3,
        scratch_shapes=[
            dma((3,)),
            dma((n - 1, 2, CHUNKS)),
            dma((n - 1, 2, CHUNKS)),
            dma((2, n - 1)),
            dma((2, n - 1)),
            dma((max(m // 2 - 1, 1),)),
            dma((max(m // 2 - 1, 1),)),
            dma((m // 2,)),
            dma((m // 2,)),
        ],
        compiler_params=pltpu.CompilerParams(
            collective_id=0, has_side_effects=True, vmem_limit_bytes=40 * 1024 * 1024
        ),
        cost_estimate=pl.CostEstimate(
            flops=40_000_000_000, bytes_accessed=20_000_000, transcendentals=0
        ),
        name="gather",
    )(tokens, cotangent, weight)


def scatter_kernel(
    n, m, part_ref, t_ref, gl_ref, gt_ref, gw_ref, glo_ref, rbuf, sbuf, fbuf, lbuf, rs_recv, rs_send,
    local_sem, ring_send, ring_recv, t_send, t_recv, l_send, l_recv, f_send, f_recv,
):
    me = lax.axis_index("sp")
    my_dp = lax.axis_index("dp")
    rows = gt_ref.shape[0]
    feats = t_ref.shape[3]
    part = rows // (2 * CHUNKS)
    place = ring_place(me, n)
    sides = [
        ring_member((place + 1) % n, n),
        ring_member((place + n - 1) % n, n),
    ]
    sp_peers = [(me + k) % n for k in range(1, n)]
    dp_peers = [(my_dp + k) % m for k in range(1, m)]
    greet([(s, my_dp) for s in sp_peers] + [(me, d) for d in dp_peers])

    def span(side, chunk):
        return pl.ds((side * CHUNKS + chunk) * part, part)

    def own_rows(step, side, chunk):
        goal = (place + 2 * n - 1 - step) % n if side == 0 else (place + 1 + step) % n
        start = ring_member(goal, n) * rows + (side * CHUNKS + chunk) * part
        return pl.ds(pl.multiple_of(start, part), part)

    def ring(step, side, chunk):
        if step == 0:
            src = part_ref.at[own_rows(0, side, chunk)]
        else:
            src = rs_send.at[step - 1, span(side, chunk)]
        return remote(
            src,
            rs_recv.at[step, span(side, chunk)],
            ring_send.at[step, side, chunk],
            ring_recv.at[step, side, chunk],
            sides[side],
            my_dp,
        )

    order = [(side, chunk) for chunk in range(CHUNKS) for side in range(2)]
    hops = {}
    for side, chunk in order:
        hops[0, side, chunk] = ring(0, side, chunk)
        hops[0, side, chunk].start()
    t_copies = [
        remote(t_ref.at[d], rbuf.at[k], t_send.at[k], t_recv.at[k], me, d)
        for k, d in enumerate(dp_peers)
    ]
    l_copies = [
        remote(gl_ref, lbuf.at[k], l_send.at[k], l_recv.at[k], me, d)
        for k, d in enumerate(dp_peers)
    ]
    for copy in l_copies + t_copies:
        copy.start()
    f_copies = [
        remote(sbuf.at[s], fbuf.at[me], f_send.at[k], f_recv.at[k], s, my_dp)
        for k, s in enumerate(sp_peers)
    ]
    own_f = pltpu.make_async_copy(sbuf.at[me], fbuf.at[me], local_sem.at[0])
    for step in range(1, n):
        for side, chunk in order:
            hops[step - 1, side, chunk].wait_recv()
            total = rs_recv[step - 1, span(side, chunk)].astype(F32)
            total = total + part_ref[own_rows(step, side, chunk)].astype(F32)
            if step < n - 1:
                rs_send[step - 1, span(side, chunk)] = total.astype(BF16)
                hops[step, side, chunk] = ring(step, side, chunk)
                hops[step, side, chunk].start()
            else:
                gt_ref[span(side, chunk)] = total.astype(BF16)
        if step == n // 2 - 1:
            for copy in t_copies:
                copy.wait_recv()
            term = t_ref[my_dp].astype(F32)
            for k in range(m - 1):
                term = term + rbuf[k].astype(F32)
            sbuf[...] = term.astype(BF16)
            for copy in f_copies:
                copy.start()
            own_f.start()
    for copy in l_copies:
        copy.wait_recv()
    lam = gl_ref[...]
    for k in range(m - 1):
        lam = lam + lbuf[k]
    glo_ref[...] = lam
    own_f.wait()
    for copy in f_copies:
        copy.wait_recv()
    for s in range(n):
        gw_ref[:, s * feats : (s + 1) * feats] = fbuf[s].astype(F32)
    for copy in list(hops.values()) + l_copies + t_copies + f_copies:
        copy.wait_send()


def scatter(partial, term, grad_lambda, n, m):
    length, depth = partial.shape
    row_count, feats = term.shape[2:]
    rows = length // n
    vmem = pl.BlockSpec(memory_space=pltpu.VMEM)
    dma = pltpu.SemaphoreType.DMA
    return pl.pallas_call(
        functools.partial(scatter_kernel, n, m),
        out_shape=[
            jax.ShapeDtypeStruct((rows, depth), BF16),
            jax.ShapeDtypeStruct((row_count, n * feats), F32),
            jax.ShapeDtypeStruct(grad_lambda.shape, F32),
        ],
        in_specs=[vmem] * 3,
        out_specs=[vmem] * 3,
        scratch_shapes=[
            pltpu.VMEM((m - 1,) + term.shape[1:], BF16),
            pltpu.VMEM(term.shape[1:], BF16),
            pltpu.VMEM(term.shape[1:], BF16),
            pltpu.VMEM((m - 1,) + grad_lambda.shape, F32),
            pltpu.VMEM((n - 1, rows, depth), BF16),
            pltpu.VMEM((max(n - 2, 1), rows, depth), BF16),
            dma((1,)),
            dma((n - 1, 2, CHUNKS)),
            dma((n - 1, 2, CHUNKS)),
            dma((m - 1,)),
            dma((m - 1,)),
            dma((m - 1,)),
            dma((m - 1,)),
            dma((n - 1,)),
            dma((n - 1,)),
        ],
        compiler_params=pltpu.CompilerParams(
            collective_id=1, has_side_effects=True, vmem_limit_bytes=48 * 1024 * 1024
        ),
        name="scatter",
    )(partial, term, grad_lambda)


def body(n, m, tokens, cotangent, value_weight, query_heads, key_heads, lambdas):
    row_count, feature_count = value_weight.shape
    all_tokens, cotan_heads, weight_cols = gather(tokens[0], cotangent[0], value_weight, n, m)
    feats = feature_count // n
    depth = n * m * row_count
    length = all_tokens.shape[0] * all_tokens.shape[1]
    head_count, width = query_heads.shape[2], query_heads.shape[3]
    flat_tokens = all_tokens.reshape(length, depth)
    weight_cols = weight_cols.reshape(depth, feats)
    values = jnp.dot(flat_tokens, weight_cols, preferred_element_type=F32).astype(BF16)
    grad_query, grad_key, grad_value, grad_lambda = attention(
        lambdas,
        query_heads.reshape(length, feats),
        key_heads.reshape(length, feats),
        values,
        cotan_heads.reshape(length, feats),
        width,
    )
    term = lax.dot_general(
        flat_tokens, grad_value, (((0,), (0,)), ((), ())), preferred_element_type=F32
    ).astype(BF16)
    term = term.reshape(n, m, row_count, feats).transpose(1, 0, 2, 3)
    partial = dot_nt(grad_value, weight_cols).astype(BF16)
    grad_tokens, grad_weight, lambda_sum = scatter(partial, term, grad_lambda, n, m)
    return (
        grad_query.reshape(1, length, head_count, width),
        grad_key.reshape(1, length, head_count, width),
        grad_tokens[None],
        grad_weight,
        lambda_sum[:, 0, 0],
    )


def solution(mesh):
    placed = (
        P("dp", "sp", None),
        P("dp", "sp", None),
        P(("sp", "dp"), None),
        P("dp", None, "sp", None),
        P("dp", None, "sp", None),
        P("sp"),
    )
    return jax.shard_map(
        functools.partial(body, mesh.shape["sp"], mesh.shape["dp"]),
        mesh=mesh,
        in_specs=placed,
        out_specs=(
            P("dp", None, "sp", None),
            P("dp", None, "sp", None),
            P("dp", "sp", None),
            P(("sp", "dp"), None),
            P("sp"),
        ),
        check_vma=False,
    )
```

```python
import functools

import jax
import jax.numpy as jnp
from jax import lax
from jax.experimental import pallas as pl
from jax.experimental.pallas import tpu as pltpu
from jax.sharding import PartitionSpec as P

QBLOCK = 256
EPS = 1e-06
NEGATIVE = -1e30
CHUNKS = 4
F32 = jnp.float32
BF16 = jnp.bfloat16


def dot_nn(a, b):
    return jnp.dot(a, b, preferred_element_type=F32)


def dot_nt(a, b):
    return lax.dot_general(a, b, (((1,), (1,)), ((), ())), preferred_element_type=F32)


def attention_kernel(
    lam_ref, q_ref, k_ref, v_ref, g_ref, gq_ref, gk_ref, gv_ref, gl_ref, gk_acc, gv_acc
):
    length, width = q_ref.shape
    half = width // 2
    block = min(QBLOCK, length)
    scaling = half ** (-0.5)
    lam = lam_ref[pl.program_id(0)]
    lanes = lax.broadcasted_iota(jnp.int32, (length, width), 1)
    first_half = lanes < half
    q_all = q_ref[...].astype(F32) * scaling
    k_all = k_ref[...].astype(F32) * scaling
    q_halves = [
        jnp.where(first_half, q_all, 0.0).astype(BF16),
        jnp.where(first_half, 0.0, q_all).astype(BF16),
    ]
    kt_halves = [
        jnp.where(first_half, k_all, 0.0).T.astype(BF16),
        jnp.where(first_half, 0.0, k_all).T.astype(BF16),
    ]
    vt = v_ref[...].astype(F32).T.astype(BF16)
    gt = g_ref[...].astype(F32).T
    keep = lax.broadcasted_iota(jnp.int32, (block, block), 0) <= lax.broadcasted_iota(
        jnp.int32, (block, block), 1
    )
    lambda_total = jnp.zeros((1, block), F32)
    for index in range(length // block):
        off = index * block
        reach = off + block
        pieces = ([(0, off)] if off else []) + [(off, reach)]
        probs = []
        for c in range(2):
            qc = q_halves[c][off:reach]
            scores = [dot_nt(k_ref[lo:hi], qc) for lo, hi in pieces]
            scores[-1] = jnp.where(keep, scores[-1], NEGATIVE)
            top = functools.reduce(
                jnp.maximum, [jnp.max(s, axis=0, keepdims=True) for s in scores]
            )
            exps = [jnp.exp(s - top) for s in scores]
            total = sum(jnp.sum(e, axis=0, keepdims=True) for e in exps)
            inv = 1.0 / total
            probs.append([e * inv for e in exps])
        weights = [(p1 - lam * p2).astype(BF16) for p1, p2 in zip(*probs)]
        out_t = sum(dot_nn(vt[:, lo:hi], w) for (lo, hi), w in zip(pieces, weights))
        cot = gt[:, off:reach]
        inverse = lax.rsqrt(jnp.mean(out_t * out_t, axis=0, keepdims=True) + EPS)
        normed = out_t * inverse
        grad_out = (
            inverse * (cot - normed * jnp.mean(cot * normed, axis=0, keepdims=True))
        ).astype(BF16)
        grad_w = [dot_nn(v_ref[lo:hi], grad_out) for lo, hi in pieces]
        sums = [
            sum(jnp.sum(d * p, axis=0, keepdims=True) for d, p in zip(grad_w, probs[c]))
            for c in range(2)
        ]
        lambda_total = lambda_total - sums[1]
        first = [(p * (d - sums[0])).astype(BF16) for d, p in zip(grad_w, probs[0])]
        second = [(-lam * p * (d - sums[1])).astype(BF16) for d, p in zip(grad_w, probs[1])]
        gq_t = sum(
            dot_nn(kt_halves[0][:, lo:hi], a) + dot_nn(kt_halves[1][:, lo:hi], b)
            for (lo, hi), a, b in zip(pieces, first, second)
        )
        gq_ref[off:reach, :] = gq_t.T.astype(BF16)
        for (lo, hi), w, a, b in zip(pieces, weights, first, second):
            gv = dot_nt(w, grad_out)
            gk = dot_nn(a, q_halves[0][off:reach]) + dot_nn(b, q_halves[1][off:reach])
            if lo == off:
                gv_acc[lo:hi, :] = gv
                gk_acc[lo:hi, :] = gk
            else:
                gv_acc[lo:hi, :] += gv
                gk_acc[lo:hi, :] += gk
    gk_ref[...] = gk_acc[...].astype(BF16)
    gv_ref[...] = gv_acc[...].astype(BF16)
    gl_ref[...] = jnp.broadcast_to(jnp.sum(lambda_total, axis=1, keepdims=True), gl_ref.shape[1:])[
        None
    ]


def attention(lambdas, queries, keys, values, cotangent, width):
    length, features = queries.shape
    heads = features // width
    column = pl.BlockSpec((length, width), lambda h: (0, h))
    shape = jax.ShapeDtypeStruct((length, features), BF16)
    return pl.pallas_call(
        attention_kernel,
        grid=(heads,),
        in_specs=[pl.BlockSpec(memory_space=pltpu.SMEM)] + [column] * 4,
        out_specs=[column] * 3 + [pl.BlockSpec((1, 8, 128), lambda h: (h, 0, 0))],
        out_shape=[shape] * 3 + [jax.ShapeDtypeStruct((heads, 8, 128), F32)],
        scratch_shapes=[pltpu.VMEM((length, width), F32)] * 2,
        compiler_params=pltpu.CompilerParams(vmem_limit_bytes=48 * 1024 * 1024),
        cost_estimate=pl.CostEstimate(
            flops=12 * length * length * width * heads,
            bytes_accessed=14 * length * features,
            transcendentals=length * length * heads,
        ),
        name="attention",
    )(lambdas, queries, keys, values, cotangent)


def remote(src, dst, send, recv, sp, dp):
    return pltpu.make_async_remote_copy(
        src_ref=src,
        dst_ref=dst,
        send_sem=send,
        recv_sem=recv,
        device_id=(sp, dp),
        device_id_type=pl.DeviceIdType.MESH,
    )


def ring_place(sp, n):
    odd = sp % 2
    return (1 - odd) * (sp // 2) + odd * (n - 1 - sp // 2)


def ring_member(place, n):
    late = place // (n // 2)
    return (1 - late) * (2 * place) + late * (2 * (n - 1 - place) + 1)


def greet(peers):
    barrier = pltpu.get_barrier_semaphore()
    for sp, dp in peers:
        pl.semaphore_signal(
            barrier, inc=1, device_id=(sp, dp), device_id_type=pl.DeviceIdType.MESH
        )
    pl.semaphore_wait(barrier, len(peers))


def gather_kernel(
    n,
    m,
    tok_ref,
    cot_ref,
    w_ref,
    all_ref,
    coth_ref,
    wc_ref,
    local_sem,
    ring_send,
    ring_recv,
    a_send,
    a_recv,
    x_send,
    x_recv,
    c_send,
    c_recv,
):
    me = lax.axis_index("sp")
    my_dp = lax.axis_index("dp")
    rows = tok_ref.shape[0]
    feats = coth_ref.shape[2]
    part = rows // (2 * CHUNKS)
    place = ring_place(me, n)
    sides = [
        ring_member((place + 1) % n, n),
        ring_member((place + n - 1) % n, n),
    ]
    core = my_dp + 1 - 2 * (my_dp % 2)
    sp_peers = [(me + k) % n for k in range(1, n)]
    x_peers = [(my_dp + 2 * k) % m for k in range(1, m // 2)]
    greet(
        [(s, my_dp) for s in sp_peers] + [(me, d) for d in x_peers] + [(me, core)]
    )

    def columns(ref, s):
        return ref.at[:, pl.ds(pl.multiple_of(s * feats, feats), feats)]

    w_copies = [
        remote(columns(w_ref, s), wc_ref.at[me, my_dp], a_send.at[0, k], a_recv.at[0, k], s, my_dp)
        for k, s in enumerate(sp_peers)
    ]
    for copy in w_copies:
        copy.start()

    def ring(step, side, chunk):
        origin = (place + n - step) % n if side == 0 else (place + step) % n
        block = ring_member(origin, n)
        span = pl.ds((side * CHUNKS + chunk) * part, part)
        src = tok_ref.at[span] if step == 0 else all_ref.at[block, span]
        return remote(
            src,
            all_ref.at[block, span],
            ring_send.at[step, side, chunk],
            ring_recv.at[step, side, chunk],
            sides[side],
            my_dp,
        )

    order = [(side, chunk) for chunk in range(CHUNKS) for side in range(2)]
    hops = {}
    for side, chunk in order:
        hops[0, side, chunk] = ring(0, side, chunk)
        hops[0, side, chunk].start()
    locals_ = [
        pltpu.make_async_copy(tok_ref, all_ref.at[me], local_sem.at[0]),
        pltpu.make_async_copy(columns(cot_ref, me), coth_ref.at[me], local_sem.at[1]),
        pltpu.make_async_copy(columns(w_ref, me), wc_ref.at[me, my_dp], local_sem.at[2]),
    ]
    for copy in locals_:
        copy.start()
    cot_copies = [
        remote(columns(cot_ref, s), coth_ref.at[me], a_send.at[1, k], a_recv.at[1, k], s, my_dp)
        for k, s in enumerate(sp_peers)
    ]
    for copy in cot_copies:
        copy.start()
    locals_[2].wait()
    for copy in w_copies:
        copy.wait_recv()
    x_copies = [
        remote(wc_ref.at[:, my_dp], wc_ref.at[:, my_dp], x_send.at[k], x_recv.at[k], me, d)
        for k, d in enumerate(x_peers)
    ]
    for copy in x_copies:
        copy.start()
    c_copies = [remote(wc_ref.at[:, my_dp], wc_ref.at[:, my_dp], c_send.at[0], c_recv.at[0], me, core)]
    c_copies[0].start()
    for step in range(1, n - 1):
        for side, chunk in order:
            hops[step - 1, side, chunk].wait_recv()
            hops[step, side, chunk] = ring(step, side, chunk)
            hops[step, side, chunk].start()
        if step == n // 2:
            for k in range(1, m // 2):
                origin = (my_dp + m - 2 * k) % m
                x_copies[k - 1].wait_recv()
                copy = remote(
                    wc_ref.at[:, origin], wc_ref.at[:, origin], c_send.at[k], c_recv.at[k], me, core
                )
                copy.start()
                c_copies.append(copy)
    for side, chunk in order:
        hops[n - 2, side, chunk].wait_recv()
    for copy in cot_copies + c_copies:
        copy.wait_recv()
    for copy in list(hops.values()) + w_copies + cot_copies + x_copies + c_copies:
        copy.wait_send()
    locals_[0].wait()
    locals_[1].wait()


def gather(tokens, cotangent, weight, n, m):
    rows, depth = tokens.shape
    feats = weight.shape[1] // n
    vmem = pl.BlockSpec(memory_space=pltpu.VMEM)
    dma = pltpu.SemaphoreType.DMA
    return pl.pallas_call(
        functools.partial(gather_kernel, n, m),
        out_shape=[
            jax.ShapeDtypeStruct((n, rows, depth), BF16),
            jax.ShapeDtypeStruct((n, rows, feats), BF16),
            jax.ShapeDtypeStruct((n, m, weight.shape[0], feats), BF16),
        ],
        in_specs=[pl.BlockSpec(memory_space=pl.ANY)] * 3,
        out_specs=[vmem] * 3,
        scratch_shapes=[
            dma((3,)),
            dma((n - 1, 2, CHUNKS)),
            dma((n - 1, 2, CHUNKS)),
            dma((2, n - 1)),
            dma((2, n - 1)),
            dma((max(m // 2 - 1, 1),)),
            dma((max(m // 2 - 1, 1),)),
            dma((m // 2,)),
            dma((m // 2,)),
        ],
        compiler_params=pltpu.CompilerParams(
            collective_id=0, has_side_effects=True, vmem_limit_bytes=60 * 1024 * 1024
        ),
        cost_estimate=pl.CostEstimate(
            flops=40_000_000_000, bytes_accessed=20_000_000, transcendentals=0
        ),
        name="gather",
    )(tokens, cotangent, weight)


def scatter_kernel(
    n, m, part_ref, t_ref, gl_ref, gt_ref, gw_ref, glo_ref, rbuf, sbuf, fbuf, lbuf, rs_recv, rs_send,
    local_sem, ring_send, ring_recv, t_send, t_recv, l_send, l_recv, f_send, f_recv,
):
    me = lax.axis_index("sp")
    my_dp = lax.axis_index("dp")
    rows = gt_ref.shape[0]
    feats = t_ref.shape[3]
    part = rows // (2 * CHUNKS)
    place = ring_place(me, n)
    sides = [
        ring_member((place + 1) % n, n),
        ring_member((place + n - 1) % n, n),
    ]
    sp_peers = [(me + k) % n for k in range(1, n)]
    dp_peers = [(my_dp + k) % m for k in range(1, m)]
    greet([(s, my_dp) for s in sp_peers] + [(me, d) for d in dp_peers])

    def span(side, chunk):
        return pl.ds((side * CHUNKS + chunk) * part, part)

    def own_rows(step, side, chunk):
        goal = (place + 2 * n - 1 - step) % n if side == 0 else (place + 1 + step) % n
        start = ring_member(goal, n) * rows + (side * CHUNKS + chunk) * part
        return pl.ds(pl.multiple_of(start, part), part)

    def ring(step, side, chunk):
        if step == 0:
            src = part_ref.at[own_rows(0, side, chunk)]
        else:
            src = rs_send.at[step - 1, span(side, chunk)]
        return remote(
            src,
            rs_recv.at[step, span(side, chunk)],
            ring_send.at[step, side, chunk],
            ring_recv.at[step, side, chunk],
            sides[side],
            my_dp,
        )

    order = [(side, chunk) for chunk in range(CHUNKS) for side in range(2)]
    hops = {}
    for side, chunk in order:
        hops[0, side, chunk] = ring(0, side, chunk)
        hops[0, side, chunk].start()
    t_copies = [
        remote(t_ref.at[d], rbuf.at[k], t_send.at[k], t_recv.at[k], me, d)
        for k, d in enumerate(dp_peers)
    ]
    l_copies = [
        remote(gl_ref, lbuf.at[k], l_send.at[k], l_recv.at[k], me, d)
        for k, d in enumerate(dp_peers)
    ]
    for copy in l_copies + t_copies:
        copy.start()
    f_copies = [
        remote(sbuf.at[s], fbuf.at[me], f_send.at[k], f_recv.at[k], s, my_dp)
        for k, s in enumerate(sp_peers)
    ]
    own_f = pltpu.make_async_copy(sbuf.at[me], fbuf.at[me], local_sem.at[0])
    for step in range(1, n):
        for side, chunk in order:
            hops[step - 1, side, chunk].wait_recv()
            total = rs_recv[step - 1, span(side, chunk)].astype(F32)
            total = total + part_ref[own_rows(step, side, chunk)].astype(F32)
            if step < n - 1:
                rs_send[step - 1, span(side, chunk)] = total.astype(BF16)
                hops[step, side, chunk] = ring(step, side, chunk)
                hops[step, side, chunk].start()
            else:
                gt_ref[span(side, chunk)] = total.astype(BF16)
        if step == n // 2 - 1:
            for copy in t_copies:
                copy.wait_recv()
            term = t_ref[my_dp].astype(F32)
            for k in range(m - 1):
                term = term + rbuf[k].astype(F32)
            sbuf[...] = term.astype(BF16)
            for copy in f_copies:
                copy.start()
            own_f.start()
    for copy in l_copies:
        copy.wait_recv()
    lam = gl_ref[...]
    for k in range(m - 1):
        lam = lam + lbuf[k]
    glo_ref[...] = lam
    own_f.wait()
    for copy in f_copies:
        copy.wait_recv()
    for s in range(n):
        gw_ref[:, s * feats : (s + 1) * feats] = fbuf[s].astype(F32)
    for copy in list(hops.values()) + l_copies + t_copies + f_copies:
        copy.wait_send()


def scatter(partial, term, grad_lambda, n, m):
    length, depth = partial.shape
    row_count, feats = term.shape[2:]
    rows = length // n
    vmem = pl.BlockSpec(memory_space=pltpu.VMEM)
    dma = pltpu.SemaphoreType.DMA
    return pl.pallas_call(
        functools.partial(scatter_kernel, n, m),
        out_shape=[
            jax.ShapeDtypeStruct((rows, depth), BF16),
            jax.ShapeDtypeStruct((row_count, n * feats), F32),
            jax.ShapeDtypeStruct(grad_lambda.shape, F32),
        ],
        in_specs=[vmem] * 3,
        out_specs=[vmem] * 3,
        scratch_shapes=[
            pltpu.VMEM((m - 1,) + term.shape[1:], BF16),
            pltpu.VMEM(term.shape[1:], BF16),
            pltpu.VMEM(term.shape[1:], BF16),
            pltpu.VMEM((m - 1,) + grad_lambda.shape, F32),
            pltpu.VMEM((n - 1, rows, depth), BF16),
            pltpu.VMEM((max(n - 2, 1), rows, depth), BF16),
            dma((1,)),
            dma((n - 1, 2, CHUNKS)),
            dma((n - 1, 2, CHUNKS)),
            dma((m - 1,)),
            dma((m - 1,)),
            dma((m - 1,)),
            dma((m - 1,)),
            dma((n - 1,)),
            dma((n - 1,)),
        ],
        compiler_params=pltpu.CompilerParams(
            collective_id=1, has_side_effects=True, vmem_limit_bytes=48 * 1024 * 1024
        ),
        name="scatter",
    )(partial, term, grad_lambda)


def body(n, m, tokens, cotangent, value_weight, query_heads, key_heads, lambdas):
    row_count, feature_count = value_weight.shape
    all_tokens, cotan_heads, weight_cols = gather(tokens[0], cotangent[0], value_weight, n, m)
    feats = feature_count // n
    depth = n * m * row_count
    length = all_tokens.shape[0] * all_tokens.shape[1]
    head_count, width = query_heads.shape[2], query_heads.shape[3]
    flat_tokens = all_tokens.reshape(length, depth)
    weight_cols = weight_cols.reshape(depth, feats)
    values = jnp.dot(flat_tokens, weight_cols, preferred_element_type=F32).astype(BF16)
    grad_query, grad_key, grad_value, grad_lambda = attention(
        lambdas,
        query_heads.reshape(length, feats),
        key_heads.reshape(length, feats),
        values,
        cotan_heads.reshape(length, feats),
        width,
    )
    term = lax.dot_general(
        flat_tokens, grad_value, (((0,), (0,)), ((), ())), preferred_element_type=F32
    ).astype(BF16)
    term = term.reshape(n, m, row_count, feats).transpose(1, 0, 2, 3)
    partial = dot_nt(grad_value, weight_cols).astype(BF16)
    grad_tokens, grad_weight, lambda_sum = scatter(partial, term, grad_lambda, n, m)
    return (
        grad_query.reshape(1, length, head_count, width),
        grad_key.reshape(1, length, head_count, width),
        grad_tokens[None],
        grad_weight,
        lambda_sum[:, 0, 0],
    )


def solution(mesh):
    placed = (
        P("dp", "sp", None),
        P("dp", "sp", None),
        P(("sp", "dp"), None),
        P("dp", None, "sp", None),
        P("dp", None, "sp", None),
        P("sp"),
    )
    return jax.shard_map(
        functools.partial(body, mesh.shape["sp"], mesh.shape["dp"]),
        mesh=mesh,
        in_specs=placed,
        out_specs=(
            P("dp", None, "sp", None),
            P("dp", None, "sp", None),
            P("dp", "sp", None),
            P(("sp", "dp"), None),
            P("sp"),
        ),
        check_vma=False,
    )
```
